512 devices in a mesh: grp: 2 (over y), fs: 32 (over z), tp: 8 (over x, core).
Axes of the slice: x: 4, y: 2, z: 32, core: 2. Of those that a mesh axis runs over, the one named last changes fastest.
The devices are a block of a 4x8x32 slice.
Arguments:
- tokens: bfloat16 [24576, 2048], P(('grp', 'fs'), 'tp'), parts along dimension 0, may hold values from -6 to 6
- norm_gain: float32 [2048], P('fs'), may hold values from 0.1 to 1.9
- gate_weight: float32 [32, 2048, 1024], P(None, 'fs', 'tp'), may hold values from -0.125 to 0.125
- up_weight: float32 [32, 2048, 1024], P(None, 'fs', 'tp'), may hold values from -0.125 to 0.125
- down_weight: float32 [32, 2048, 1024], P(None, 'fs', 'tp'), may hold values from -0.5 to 0.5
- expert_ids: int32 [24576, 2], P(('grp', 'fs')), parts along dimension 0, may hold values from 0 to 31, as said below
- group_logits: float32 [24576, 2], P(('grp', 'fs')), parts along dimension 0, may hold values from -2.5 to 2.5
- pair_logits: float32 [24576, 2], P(('grp', 'fs')), parts along dimension 0, may hold values from -2.5 to 2.5
Outputs:
- mixed: bfloat16 [24576, 2048], P(('grp', 'fs'), 'tp'), parts along dimension 0
- gate_out: bfloat16 [64, 2048, 1024], P(('grp', 'fs'), None, 'tp'), parts along dimension 0
- up_out: bfloat16 [64, 2048, 1024], P(('grp', 'fs'), None, 'tp'), parts along dimension 0
- down_out: bfloat16 [64, 2048, 1024], P(('grp', 'fs'), None, 'tp'), parts along dimension 0
The draws below stay inside these ranges and needn't reach their ends.
There are 2 independent parts, one for each index of `grp`. The reference program is written for one: setup_inputs(seed, part) draws one part's arguments, and reference() takes and returns one part's arrays. A program takes and returns all parts, laid end to end along the dimension named above; an argument that names none is the same for every part. Nothing has to cross between parts.
Inputs may be any that keep to these rules, and one draw needn't show every extreme that they name: `expert_ids`: each row names two different experts of one group: both ids lie in the same run of 16 consecutive ids.
All inputs are finite; a program needn't handle non-finite values.
Results may differ from the reference program's by a relative error of at most 0.015.
Values may be sent and summed in bfloat16 or wider, within the bound.
A program may use at most 64 MiB of HBM per device.

```python
from functools import partial
import jax
import jax.numpy as jnp
from jax import lax

D = 2048
FF = 1024
GROUPS = 2
TOP = 2
TOK_DEV = 384
EXPERTS = 32
EXP_GROUP = 16
CAP = 30
TOKENS = 12288
N_FS = 32
N_TP = 8


def pick_by_weight(key, table):
    running = jnp.cumsum(table, axis=1)
    total = running[:, -1]
    draw = jax.random.randint(key, (table.shape[0],), 0, 1 << 30) % total
    return jnp.sum((running <= draw[:, None]).astype(jnp.int32), axis=1).astype(jnp.int32)


def draw_expert_ids(key, part):
    base = jax.random.fold_in(key, 11)
    key_hot, key_first, key_second = jax.random.split(base, 3)
    block_count = TOKENS // TOK_DEV
    block_keys = jax.random.split(key_hot, block_count)
    orders = jax.vmap(lambda single: jax.random.permutation(single, EXPERTS))(block_keys)
    block_table = 1 + 2 * (orders < EXPERTS // 2).astype(jnp.int32)
    token_block = jnp.arange(TOKENS, dtype=jnp.int32) // TOK_DEV
    token_table = block_table[token_block]
    first_pick = pick_by_weight(key_first, token_table)
    columns = jnp.arange(EXPERTS, dtype=jnp.int32)
    allowed = (columns[None, :] // EXP_GROUP == (first_pick // EXP_GROUP)[:, None]) & (columns[None, :] != first_pick[:, None])
    second_table = token_table * allowed.astype(jnp.int32)
    second_pick = pick_by_weight(key_second, second_table)
    return jnp.stack([first_pick, second_pick], axis=1).astype(jnp.int32)


def draw_tokens(key, part):
    base = jax.random.fold_in(key, 21)
    raw = jnp.clip(jax.random.normal(base, (TOKENS, D), jnp.float32), -3.0, 3.0)
    factor = 1.0 / jnp.sqrt(jnp.mean(raw * raw, axis=1, keepdims=True) + 1e-06)
    return jnp.clip(raw * factor, -6.0, 6.0).astype(jnp.bfloat16)


def draw_group_logits(key, part):
    base = jax.random.fold_in(key, 31)
    values = jnp.clip(0.6 * jax.random.normal(base, (TOKENS, GROUPS), jnp.float32), -2.5, 2.5)
    return values.astype(jnp.float32)


def draw_pair_logits(key, part):
    base = jax.random.fold_in(key, 41)
    values = jnp.clip(0.6 * jax.random.normal(base, (TOKENS, TOP), jnp.float32), -2.5, 2.5)
    return values.astype(jnp.float32)


def shard_levels(key, shape, cuts, low, high):
    def one(axis_at, blocks):
        steps = jax.random.uniform(jax.random.fold_in(jax.random.fold_in(key, 6), axis_at), (blocks,), jnp.float32, low / len(cuts), high / len(cuts))
        return jnp.repeat(jnp.exp(steps), shape[axis_at] // blocks).reshape((-1,) + (1,) * (len(shape) - axis_at - 1))

    level = one(*cuts[0])
    for cut in cuts[1:]:
        level = level * one(*cut)
    return level


def bell_draw(rng, extent, scale, most, cuts=(), kind=jnp.bfloat16):
    values = jax.random.normal(rng, extent, jnp.float32) * scale
    if len(cuts) > 0:
        values = shard_levels(rng, extent, cuts, -0.22, 0.18) * values
    return jnp.clip(values, min=-most, max=most).astype(kind)


def setup_inputs(seed: int = 0, part: int = 0) -> dict:
    key_of = jax.random.split(jax.random.key(seed), 9)
    own_keys = jax.random.split(jax.random.fold_in(key_of[8], part), 9)
    tokens = draw_tokens(jax.random.fold_in(jax.random.fold_in(key_of[8], part), 71), part)
    norm_gain = jnp.clip(1.0 + 0.18 * jax.random.normal(key_of[1], (D,), jnp.float32), 0.1, 1.9)
    gate_weight = bell_draw(key_of[2], (EXPERTS, D, FF), D ** -0.5, 0.125, ((1, 32), (2, 8)), jnp.float32)
    up_weight = bell_draw(key_of[3], (EXPERTS, D, FF), D ** -0.5, 0.125, ((1, 32), (2, 8)), jnp.float32)
    down_weight = bell_draw(key_of[4], (EXPERTS, D, FF), (FF // 8) ** -0.5, 0.5, ((1, 32), (2, 8)), jnp.float32)
    expert_ids = draw_expert_ids(jax.random.fold_in(jax.random.fold_in(key_of[8], part), 71), part)
    group_logits = draw_group_logits(jax.random.fold_in(jax.random.fold_in(key_of[8], part), 71), part)
    pair_logits = draw_pair_logits(jax.random.fold_in(jax.random.fold_in(key_of[8], part), 71), part)
    return dict(tokens=tokens, norm_gain=norm_gain, gate_weight=gate_weight, up_weight=up_weight, down_weight=down_weight, expert_ids=expert_ids, group_logits=group_logits, pair_logits=pair_logits)


def routing(block_ids, experts, capacity):
    entries = block_ids.reshape(-1).astype(jnp.int32)
    onehot = (entries[:, None] == jnp.arange(experts, dtype=jnp.int32)[None, :]).astype(jnp.int32)
    before = jnp.cumsum(onehot, axis=0) - onehot
    entry_rank = jnp.sum(before * onehot, axis=1)
    kept = entry_rank < capacity
    slot_index = jnp.where(kept, entries * capacity + entry_rank, experts * capacity)
    return slot_index.astype(jnp.int32), kept


def fill_slots(block_rows, slot_index, experts, capacity):
    entry_count = slot_index.shape[0]
    source_row = jnp.arange(entry_count, dtype=jnp.int32) // 2
    slot_row = jnp.zeros((experts * capacity + 1,), jnp.int32).at[slot_index].set(source_row)
    filled = jnp.zeros((experts * capacity + 1,), jnp.float32).at[slot_index].set(1.0)
    chosen = block_rows[slot_row[:experts * capacity]]
    return chosen * filled[:experts * capacity, None].astype(block_rows.dtype)


def route_weights(block_ids, group_logits, pair_logits, kept, exp_group):
    group_pick = block_ids[:, 0] // exp_group
    group_exp = jnp.exp(group_logits)
    columns = jnp.arange(group_logits.shape[1], dtype=jnp.int32)
    chosen = jnp.sum(jnp.where(columns[None, :] == group_pick[:, None], group_exp, 0.0), axis=1)
    chosen = chosen / jnp.sum(group_exp, axis=1)
    pair_exp = jnp.exp(pair_logits)
    weights = pair_exp / jnp.sum(pair_exp, axis=1, keepdims=True) * chosen[:, None]
    return weights * kept.reshape(-1, 2).astype(weights.dtype)


def expert_apply(operands):
    slot_rows, gate_matrix, up_matrix, down_matrix = operands
    gate = jnp.dot(slot_rows, gate_matrix, preferred_element_type=jnp.float32)
    up_part = jnp.dot(slot_rows, up_matrix, preferred_element_type=jnp.float32)
    hidden = (jax.nn.silu(gate) * up_part).astype(jnp.bfloat16)
    width = FF // N_TP
    total = jnp.zeros((slot_rows.shape[0], D), jnp.float32)
    for column in range(N_TP):
        term = lax.dot_general(hidden[:, column * width:(column + 1) * width],
                               down_matrix[:, column * width:(column + 1) * width],
                               (((1,), (1,)), ((), ())), preferred_element_type=jnp.float32)
        rounded = lax.optimization_barrier(term.astype(jnp.bfloat16))
        total = total + rounded.astype(jnp.float32)
    return total.astype(jnp.bfloat16)


def combine_block(returned, slot_index, weights):
    limit = returned.shape[0] - 1
    picked = returned[jnp.clip(slot_index, 0, limit)].astype(jnp.float32)
    picked = picked.reshape(weights.shape[0], 2, -1)
    return jnp.sum(picked * weights[:, :, None], axis=1).astype(jnp.bfloat16)


def reference(tokens, norm_gain, gate_weight, up_weight, down_weight, expert_ids, group_logits, pair_logits):
    scaled = norm_gain[None, :, None]
    gate_out = (scaled * gate_weight).astype(jnp.bfloat16)
    up_out = (scaled * up_weight).astype(jnp.bfloat16)
    down_out = down_weight.astype(jnp.bfloat16)
    id_blocks = expert_ids.reshape(N_FS, TOK_DEV, 2)
    token_blocks = tokens.reshape(N_FS, TOK_DEV, D)
    slot_index, kept = jax.vmap(partial(routing, experts=EXPERTS, capacity=CAP))(id_blocks)
    buffers = jax.vmap(partial(fill_slots, experts=EXPERTS, capacity=CAP))(token_blocks, slot_index)
    buffers = buffers.reshape(N_FS, EXPERTS, CAP, D).transpose(1, 0, 2, 3).reshape(EXPERTS, N_FS * CAP, D)
    results = lax.map(expert_apply, (buffers, gate_out, up_out, down_out))
    results = results.reshape(EXPERTS, N_FS, CAP, D).transpose(1, 0, 2, 3).reshape(N_FS, EXPERTS * CAP, D)
    weights = jax.vmap(partial(route_weights, exp_group=EXP_GROUP))(
        id_blocks, group_logits.reshape(N_FS, TOK_DEV, -1), pair_logits.reshape(N_FS, TOK_DEV, 2), kept)
    mixed = jax.vmap(combine_block)(results, slot_index, weights)
    return (mixed.reshape(TOKENS, D), gate_out, up_out, down_out)
```

```python
import functools

import jax
import jax.numpy as jnp
from jax import lax
from jax.experimental import pallas as pl
from jax.experimental.pallas import tpu as pltpu
from jax.sharding import PartitionSpec as P

MESH = pl.DeviceIdType.MESH
BF = jnp.bfloat16
F32 = jnp.float32


def kernel(
    cfg, tok_hbm, gain, gate_hbm, up_hbm, down_hbm, ids, glog, plog,
    mixed, gate_o, up_o, down_o,
    wf, wstage, wbuf, wother, gu, dn, tokv, outs, trecv, piece, part, rsbuf, res, ret, onehot, cols,
    lsem, osem, ws, wr, ts, tr, rs, rr, ys, yr, ds, dr, ags, agr, rss, rsr,
):
    n, groups, tps, cap, slots, nq, ck = cfg
    half = n // 2
    tok_rows, width = tokv.shape
    me, grp, tp = lax.axis_index("fs"), lax.axis_index("grp"), lax.axis_index("tp")
    core = lax.rem(tp, 2)
    partner = tp + 1 - 2 * core

    loads = [
        pltpu.make_async_copy(src.at[:, grp], wf.at[i], lsem.at[i])
        for i, src in enumerate((gate_hbm, up_hbm, down_hbm))
    ]
    for load in loads:
        load.start()
    tok_load = pltpu.make_async_copy(tok_hbm, tokv, lsem.at[3])
    tok_load.start()

    barrier = pltpu.get_barrier_semaphore()

    def greet(axis, here, size):
        def one(o, c):
            pl.semaphore_signal(
                barrier, inc=1, device_id={axis: lax.rem(here + o, size)}, device_id_type=MESH
            )
            return c

        lax.fori_loop(1, size, one, 0)

    greet("fs", me, n)
    greet("tp", tp, tps)
    greet("grp", grp, groups)

    for i, load in enumerate(loads):
        load.wait()
        if i < 2:
            wstage[:, i] = (wf[i] * gain[grp][None]).astype(BF)
        else:
            wstage[:, i] = wf[i].astype(BF)
        wbuf[i, me, grp] = wstage[me, i]

    pl.semaphore_wait(barrier, n - 1 + tps - 1 + groups - 1)

    def delta_of(h, k):
        return half - 1 - k if h == 0 else half + k

    def to(h, k):
        return lax.rem(me + delta_of(h, k), n)

    def back(h, k):
        return lax.rem(me + n - delta_of(h, k), n)

    def every(fn, lo=0, hi=half):
        def one(k, c):
            fn(0, k)
            fn(1, k)
            return c

        last = min(hi, half - 1)
        lax.fori_loop(lo, last, one, 0)
        if hi == half:
            fn(1, half - 1)

    def w_copy(h, k, dst, src):
        return pltpu.make_async_remote_copy(
            src_ref=wstage.at[dst], dst_ref=wbuf.at[:, src, grp],
            send_sem=ws.at[h, k], recv_sem=wr.at[h, k],
            device_id={"fs": dst}, device_id_type=MESH,
        )

    def t_copy(h, k, dst):
        return pltpu.make_async_remote_copy(
            src_ref=outs.at[dst], dst_ref=trecv.at[h, k],
            send_sem=ts.at[h, k], recv_sem=tr.at[h, k],
            device_id={"fs": dst}, device_id_type=MESH,
        )

    def r_copy(h, k, dst, src):
        return pltpu.make_async_remote_copy(
            src_ref=res.at[h, k], dst_ref=ret.at[src],
            send_sem=rs.at[h, k], recv_sem=rr.at[h, k],
            device_id={"fs": dst}, device_id_type=MESH,
        )

    every(lambda h, k: w_copy(h, k, to(h, k), me).start())

    exp_group = n // glog.shape[0]
    first, second = ids[0:1, :], ids[1:2, :]
    e_iota = lax.broadcasted_iota(jnp.int32, (n, tok_rows), 0)
    is0, is1 = e_iota == first, e_iota == second
    count = (is0 | is1).astype(F32).astype(BF)
    earlier = (
        lax.broadcasted_iota(jnp.int32, (tok_rows, tok_rows), 0)
        < lax.broadcasted_iota(jnp.int32, (tok_rows, tok_rows), 1)
    ).astype(F32).astype(BF)
    before = jnp.dot(count, earlier, preferred_element_type=F32)
    rank0 = jnp.sum(jnp.where(is0, before, 0.0), axis=0, keepdims=True)
    rank1 = jnp.sum(jnp.where(is1, before, 0.0), axis=0, keepdims=True)
    keep0, keep1 = rank0 < cap, rank1 < cap
    slot0 = jnp.where(keep0, first.astype(F32) * slots + rank0, -1.0)
    slot1 = jnp.where(keep1, second.astype(F32) * slots + rank1, -1.0)

    group_exp = [jnp.exp(glog[g : g + 1, :]) for g in range(glog.shape[0])]
    chosen, total = jnp.zeros_like(slot0), jnp.zeros_like(slot0)
    for g, value in enumerate(group_exp):
        mine = (first >= g * exp_group) & (first < (g + 1) * exp_group)
        chosen += jnp.where(mine, value, 0.0)
        total += value
    chosen = chosen / total
    pair0, pair1 = jnp.exp(plog[0:1, :]), jnp.exp(plog[1:2, :])
    weight0 = jnp.where(keep0, pair0 / (pair0 + pair1) * chosen, 0.0)
    weight1 = jnp.where(keep1, pair1 / (pair0 + pair1) * chosen, 0.0)

    tok_load.wait()
    tokens = tokv[...]
    slot0i, slot1i = slot0.astype(jnp.int32), slot1.astype(jnp.int32)
    build = 4 * slots
    s_iota = lax.broadcasted_iota(jnp.int32, (build, tok_rows), 0)

    def fill(b, c):
        at = s_iota + b * build
        pick = ((at == slot0i) | (at == slot1i)).astype(F32).astype(BF)
        rows = jnp.dot(pick, tokens, preferred_element_type=F32).astype(BF)
        outs[pl.ds(b * 4, 4)] = rows.reshape(4, slots, width)
        return c

    lax.fori_loop(0, n // 4, fill, 0)

    every(lambda h, k: t_copy(h, k, to(h, k)).start())
    trecv[0, half - 1] = outs[me]

    lines = lax.broadcasted_iota(jnp.int32, (128, tok_rows), 0)
    packed = jnp.zeros((128, tok_rows), F32)
    for i, row in enumerate((slot0, slot1, weight0, weight1)):
        packed = jnp.where(lines == i, row, packed)
    cols[...] = packed.T
    l_iota = lax.broadcasted_iota(jnp.int32, (tok_rows, n * slots), 1)
    for i in range(2):
        onehot[i] = (l_iota == cols[:, i : i + 1].astype(jnp.int32)).astype(F32).astype(BF)

    every(lambda h, k: w_copy(h, k, to(h, k), back(h, k)).wait_recv())

    def y_copy(o, there, whose):
        return pltpu.make_async_remote_copy(
            src_ref=wbuf.at[:, :, grp], dst_ref=wbuf.at[:, :, whose],
            send_sem=ys.at[o], recv_sem=yr.at[o],
            device_id={"grp": there}, device_id_type=MESH,
        )

    for o in range(1, groups):
        y_copy(o, lax.rem(grp + o, groups), grp).start()
    for o in range(1, groups):
        y_copy(o, lax.rem(grp + o, groups), lax.rem(grp + groups - o, groups)).wait_recv()

    exchange = pltpu.make_async_remote_copy(
        src_ref=wbuf, dst_ref=wother, send_sem=ds, recv_sem=dr,
        device_id={"tp": partner}, device_id_type=MESH,
    )
    exchange.start()
    stores = [
        pltpu.make_async_copy(wbuf.at[i], dst, osem.at[i])
        for i, dst in enumerate((gate_o, up_o, down_o))
    ]
    for store in stores:
        store.start()

    def ag_copy(q, o, there, whose):
        h = lax.rem(there, 2)
        return pltpu.make_async_remote_copy(
            src_ref=trecv.at[h, pl.ds(q * ck, ck)], dst_ref=piece.at[q, whose],
            send_sem=ags.at[q, o], recv_sem=agr.at[q, o],
            device_id={"tp": there}, device_id_type=MESH,
        )

    def rs_copy(q, o, there, whose):
        return pltpu.make_async_remote_copy(
            src_ref=part.at[q, there], dst_ref=rsbuf.at[q, whose],
            send_sem=rss.at[q, o], recv_sem=rsr.at[q, o],
            device_id={"tp": there}, device_id_type=MESH,
        )

    def ahead(o):
        return lax.rem(tp + o, tps)

    def behind(o):
        return lax.rem(tp + tps - o, tps)

    def around(fn):
        def one(o, c):
            fn(o)
            return c

        lax.fori_loop(1, tps, one, 0)

    def gather(q):
        every(lambda h, k: t_copy(h, k, to(h, k)).wait_recv(), q * ck, (q + 1) * ck)
        around(lambda o: ag_copy(q, o, ahead(o), tp).start())
        piece[q, tp] = trecv[core, q * ck : (q + 1) * ck]

    def work(q):
        around(lambda o: ag_copy(q, o, ahead(o), behind(o)).wait_recv())
        rows = ck * slots
        acc = jnp.zeros((rows, gu.shape[1]), F32)
        for j in range(tps):
            acc += jnp.dot(
                piece[q, j].reshape(rows, width), gu[j * width : (j + 1) * width, :],
                preferred_element_type=F32,
            )
        f = gu.shape[1] // 4
        hidden = []
        for i in range(2):
            gate_v, up_v = acc[:, 2 * i * f : (2 * i + 1) * f], acc[:, (2 * i + 1) * f : (2 * i + 2) * f]
            hidden.append((gate_v / (1.0 + jnp.exp(-gate_v)) * up_v).astype(BF))
        hidden = jnp.concatenate(hidden, axis=1)
        for j in range(tps):
            term = lax.dot_general(
                hidden, dn[j * width : (j + 1) * width, :], (((1,), (1,)), ((), ())),
                preferred_element_type=F32,
            )
            part[q, j] = term.astype(BF).reshape(ck, slots, width)
        around(lambda o: rs_copy(q, o, ahead(o), tp).start())
        rsbuf[q, tp] = part[q, tp]

    def finish(q):
        around(lambda o: rs_copy(q, o, ahead(o), behind(o)).wait_recv())
        for h in range(2):
            total = rsbuf[q, h].astype(F32)
            for chip in range(1, tps // 2):
                total += rsbuf[q, 2 * chip + h].astype(F32)
            res[h, q * ck : (q + 1) * ck] = total.astype(BF)
        every(lambda h, k: r_copy(h, k, back(h, k), me).start(), q * ck, (q + 1) * ck)

    gather(0)
    exchange.wait_recv()
    f = wbuf.shape[-1]
    depth = gu.shape[0]
    for i, src in enumerate((wbuf, wother)):
        gu[:, 2 * i * f : (2 * i + 1) * f] = src[0].reshape(depth, f)
        gu[:, (2 * i + 1) * f : (2 * i + 2) * f] = src[1].reshape(depth, f)
        dn[:, i * f : (i + 1) * f] = src[2].reshape(depth, f)

    todo = []
    for q in range(nq):
        todo += [(2 * q + 0.0, gather, q), (2 * q + 1.1, work, q), (2 * q + 3.2, finish, q)]
    for _, step, q in sorted(todo, key=lambda item: item[0])[1:]:
        step(q)

    ret[me] = res[0, half - 1]
    every(lambda h, k: r_copy(h, k, back(h, k), to(h, k)).wait_recv())
    table = ret[...].reshape(n * slots, width)
    mix = jnp.zeros((tok_rows, width), F32)
    for i in range(2):
        rows = jnp.dot(onehot[i], table, preferred_element_type=F32)
        mix += rows * cols[:, 2 + i : 3 + i]
    mixed[...] = mix.astype(BF)

    for store in stores:
        store.wait()
    every(lambda h, k: w_copy(h, k, to(h, k), me).wait_send())
    every(lambda h, k: t_copy(h, k, to(h, k)).wait_send())
    every(lambda h, k: r_copy(h, k, back(h, k), me).wait_send())
    for o in range(1, groups):
        y_copy(o, lax.rem(grp + o, groups), grp).wait_send()
    exchange.wait_send()
    for q in range(nq):
        around(lambda o: ag_copy(q, o, ahead(o), tp).wait_send())
        around(lambda o: rs_copy(q, o, ahead(o), tp).wait_send())


def body(chunks, tokens, norm_gain, gate_weight, up_weight, down_weight, ids, group_logits, pair_logits):
    experts, rows, f = gate_weight.shape
    tok_rows, width = tokens.shape
    n, groups, tps = lax.axis_size("fs"), lax.axis_size("grp"), lax.axis_size("tp")
    cap = 5 * tok_rows * 2 // (4 * experts)
    slots = -(-cap // 16) * 16
    half = n // 2
    ck = half // chunks
    share = rows // groups
    depth = n * rows

    def cut(weight):
        return weight.reshape(experts, groups, share, f)

    gain = jnp.broadcast_to(norm_gain[:, None], (rows, f)).reshape(groups, share, f)
    vmem = pl.BlockSpec(memory_space=pltpu.VMEM)
    hbm = pl.BlockSpec(memory_space=pl.ANY)
    whole = jax.ShapeDtypeStruct((n, groups, share, f), BF)
    dma = pltpu.SemaphoreType.DMA
    out = pl.pallas_call(
        functools.partial(kernel, (n, groups, tps, cap, slots, chunks, ck)),
        out_shape=(jax.ShapeDtypeStruct((tok_rows, width), BF), whole, whole, whole),
        in_specs=[hbm, vmem, hbm, hbm, hbm, vmem, vmem, vmem],
        out_specs=(vmem, hbm, hbm, hbm),
        scratch_shapes=[
            pltpu.VMEM((3, n, share, f), F32),
            pltpu.VMEM((n, 3, share, f), BF),
            pltpu.VMEM((3, n, groups, share, f), BF),
            pltpu.VMEM((3, n, groups, share, f), BF),
            pltpu.VMEM((depth, 4 * f), BF),
            pltpu.VMEM((depth, 2 * f), BF),
            pltpu.VMEM((tok_rows, width), BF),
            pltpu.VMEM((n, slots, width), BF),
            pltpu.VMEM((2, half, slots, width), BF),
            pltpu.VMEM((chunks, tps, ck, slots, width), BF),
            pltpu.VMEM((chunks, tps, ck, slots, width), BF),
            pltpu.VMEM((chunks, tps, ck, slots, width), BF),
            pltpu.VMEM((2, half, slots, width), BF),
            pltpu.VMEM((n, slots, width), BF),
            pltpu.VMEM((2, tok_rows, n * slots), BF),
            pltpu.VMEM((tok_rows, 128), F32),
            dma((4,)), dma((3,)),
            dma((2, half)), dma((2, half)),
            dma((2, half)), dma((2, half)),
            dma((2, half)), dma((2, half)),
            dma((groups,)), dma((groups,)),
            dma, dma,
            dma((chunks, tps)), dma((chunks, tps)),
            dma((chunks, tps)), dma((chunks, tps)),
        ],
        compiler_params=pltpu.CompilerParams(collective_id=0, has_side_effects=True),
    )(
        tokens, gain, cut(gate_weight), cut(up_weight), cut(down_weight),
        ids.T, group_logits.T, pair_logits.T,
    )
    mixed, gate_out, up_out, down_out = out
    return (mixed,) + tuple(w.reshape(1, depth, f) for w in (gate_out, up_out, down_out))


def solution(mesh, chunks=4):
    placed = (
        P(("grp", "fs"), "tp"),
        P("fs"),
        P(None, "fs", "tp"),
        P(None, "fs", "tp"),
        P(None, "fs", "tp"),
        P(("grp", "fs"), None),
        P(("grp", "fs"), None),
        P(("grp", "fs"), None),
    )
    return jax.shard_map(
        functools.partial(body, chunks),
        mesh=mesh,
        in_specs=placed,
        out_specs=(
            P(("grp", "fs"), "tp"),
            P(("grp", "fs"), None, "tp"),
            P(("grp", "fs"), None, "tp"),
            P(("grp", "fs"), None, "tp"),
        ),
        check_vma=False,
    )
```

```python
import functools

import jax
import jax.numpy as jnp
from jax import lax
from jax.experimental import pallas as pl
from jax.experimental.pallas import tpu as pltpu
from jax.sharding import PartitionSpec as P

MESH = pl.DeviceIdType.MESH
BF = jnp.bfloat16
F32 = jnp.float32


def kernel(
    cfg, tok_hbm, gain, gate_hbm, up_hbm, down_hbm, ids, glog, plog,
    mixed, gate_o, up_o, down_o,
    gains, wf, wstage, wbuf, wother, gu, dn, tokv, outs, trecv, piece, part, rsbuf, res, ret, onehot, cols,
    ready, lsem, osem, ws, wr, ts, tr, rs, rr, ys, yr, ds, dr, ags, agr, rss, rsr,
):
    n, groups, tps, cap, slots, nq, ck = cfg
    half = n // 2
    tok_rows, width = tokv.shape
    me, grp, tp = lax.axis_index("fs"), lax.axis_index("grp"), lax.axis_index("tp")
    core = lax.rem(tp, 2)
    partner = tp + 1 - 2 * core

    loads = [
        pltpu.make_async_copy(src.at[:, grp], wf.at[i], lsem.at[i])
        for i, src in enumerate((gate_hbm, up_hbm, down_hbm))
    ]
    for load in loads:
        load.start()
    tok_load = pltpu.make_async_copy(tok_hbm, tokv, lsem.at[3])
    tok_load.start()

    barrier = pltpu.get_barrier_semaphore()
    rank = lax.rem(me + n - 1, n)

    def loop(lo, hi, fn):
        def one(i, c):
            fn(i)
            return c

        lax.fori_loop(lo, hi, one, 0)

    def greet(axis, there):
        pl.semaphore_signal(barrier, inc=1, device_id={axis: there}, device_id_type=MESH)

    loop(1, n - rank, lambda i: greet("fs", lax.rem(me + i, n)))
    loop(1, tps, lambda i: greet("tp", lax.rem(tp + i, tps)))
    loop(1, groups, lambda i: greet("grp", lax.rem(grp + i, groups)))

    rows = gain.shape[1]
    diagonal = lax.broadcasted_iota(jnp.int32, (rows, rows), 0) == lax.broadcasted_iota(jnp.int32, (rows, rows), 1)
    column = jnp.sum(jnp.where(diagonal, gain[...], 0.0), axis=1, keepdims=True)
    gains[...] = jnp.broadcast_to(column, (rows, gains.shape[2])).reshape(gains.shape)
    for i, load in enumerate(loads):
        load.wait()
        if i < 2:
            wstage[:, i] = (wf[i] * gains[grp][None]).astype(BF)
        else:
            wstage[:, i] = wf[i].astype(BF)
        wbuf[i, me, grp] = wstage[me, i]

    pl.semaphore_wait(barrier, rank + tps - 1 + groups - 1)

    def report(i):
        there = lax.rem(me + n - i, n)
        pl.semaphore_signal(ready.at[i], inc=1, device_id={"fs": there}, device_id_type=MESH)

    loop(1, rank + 1, report)

    def delta_of(h, k):
        return half - 1 - k if h == 0 else half + k

    def to(h, k):
        return lax.rem(me + delta_of(h, k), n)

    def back(h, k):
        return lax.rem(me + n - delta_of(h, k), n)

    def every(fn, lo=0, hi=half):
        def one(k, c):
            fn(0, k)
            fn(1, k)
            return c

        last = min(hi, half - 1)
        lax.fori_loop(lo, last, one, 0)
        if hi == half:
            fn(1, half - 1)

    def w_copy(delta, dst, src):
        return pltpu.make_async_remote_copy(
            src_ref=wstage.at[dst], dst_ref=wbuf.at[:, src, grp],
            send_sem=ws.at[delta], recv_sem=wr.at[delta],
            device_id={"fs": dst}, device_id_type=MESH,
        )

    def w_to(delta):
        return w_copy(delta, lax.rem(me + delta, n), me)

    def w_from(delta):
        return w_copy(delta, lax.rem(me + delta, n), lax.rem(me + n - delta, n))

    def t_copy(h, k, dst):
        return pltpu.make_async_remote_copy(
            src_ref=outs.at[dst], dst_ref=trecv.at[h, k],
            send_sem=ts.at[h, k], recv_sem=tr.at[h, k],
            device_id={"fs": dst}, device_id_type=MESH,
        )

    def r_copy(h, k, dst, src):
        return pltpu.make_async_remote_copy(
            src_ref=res.at[h, k], dst_ref=ret.at[src],
            send_sem=rs.at[h, k], recv_sem=rr.at[h, k],
            device_id={"fs": dst}, device_id_type=MESH,
        )

    loop(1, rank + 1, lambda i: w_to(n - i).start())

    exp_group = n // glog.shape[0]
    first, second = ids[0:1, :], ids[1:2, :]
    e_iota = lax.broadcasted_iota(jnp.int32, (n, tok_rows), 0)
    is0, is1 = e_iota == first, e_iota == second
    count = (is0 | is1).astype(F32).astype(BF)
    earlier = (
        lax.broadcasted_iota(jnp.int32, (tok_rows, tok_rows), 0)
        < lax.broadcasted_iota(jnp.int32, (tok_rows, tok_rows), 1)
    ).astype(F32).astype(BF)
    before = jnp.dot(count, earlier, preferred_element_type=F32)
    rank0 = jnp.sum(jnp.where(is0, before, 0.0), axis=0, keepdims=True)
    rank1 = jnp.sum(jnp.where(is1, before, 0.0), axis=0, keepdims=True)
    keep0, keep1 = rank0 < cap, rank1 < cap
    slot0 = jnp.where(keep0, first.astype(F32) * slots + rank0, -1.0)
    slot1 = jnp.where(keep1, second.astype(F32) * slots + rank1, -1.0)

    group_exp = [jnp.exp(glog[g : g + 1, :]) for g in range(glog.shape[0])]
    chosen, total = jnp.zeros_like(slot0), jnp.zeros_like(slot0)
    for g, value in enumerate(group_exp):
        mine = (first >= g * exp_group) & (first < (g + 1) * exp_group)
        chosen += jnp.where(mine, value, 0.0)
        total += value
    chosen = chosen / total
    pair0, pair1 = jnp.exp(plog[0:1, :]), jnp.exp(plog[1:2, :])
    weight0 = jnp.where(keep0, pair0 / (pair0 + pair1) * chosen, 0.0)
    weight1 = jnp.where(keep1, pair1 / (pair0 + pair1) * chosen, 0.0)

    tok_load.wait()
    tokens = tokv[...]
    slot0i, slot1i = slot0.astype(jnp.int32), slot1.astype(jnp.int32)
    build = 4 * slots
    s_iota = lax.broadcasted_iota(jnp.int32, (build, tok_rows), 0)

    def fill(b, c):
        at = s_iota + b * build
        pick = ((at == slot0i) | (at == slot1i)).astype(F32).astype(BF)
        rows = jnp.dot(pick, tokens, preferred_element_type=F32).astype(BF)
        outs[pl.ds(b * 4, 4)] = rows.reshape(4, slots, width)
        return c

    lax.fori_loop(0, n // 4, fill, 0)

    def late(i):
        pl.semaphore_wait(ready.at[i], 1)
        w_to(i).start()

    loop(1, n - rank, late)
    every(lambda h, k: t_copy(h, k, to(h, k)).start())
    trecv[0, half - 1] = outs[me]

    lines = lax.broadcasted_iota(jnp.int32, (128, tok_rows), 0)
    packed = jnp.zeros((128, tok_rows), F32)
    for i, row in enumerate((slot0, slot1, weight0, weight1)):
        packed = jnp.where(lines == i, row, packed)
    cols[...] = packed.T
    l_iota = lax.broadcasted_iota(jnp.int32, (tok_rows, n * slots), 1)
    for i in range(2):
        onehot[i] = (l_iota == cols[:, i : i + 1].astype(jnp.int32)).astype(F32).astype(BF)

    loop(1, n, lambda delta: w_from(delta).wait_recv())

    def y_copy(o, there, whose):
        return pltpu.make_async_remote_copy(
            src_ref=wbuf.at[:, :, grp], dst_ref=wbuf.at[:, :, whose],
            send_sem=ys.at[o], recv_sem=yr.at[o],
            device_id={"grp": there}, device_id_type=MESH,
        )

    for o in range(1, groups):
        y_copy(o, lax.rem(grp + o, groups), grp).start()
    for o in range(1, groups):
        y_copy(o, lax.rem(grp + o, groups), lax.rem(grp + groups - o, groups)).wait_recv()

    exchange = pltpu.make_async_remote_copy(
        src_ref=wbuf, dst_ref=wother, send_sem=ds, recv_sem=dr,
        device_id={"tp": partner}, device_id_type=MESH,
    )
    exchange.start()
    stores = [
        pltpu.make_async_copy(wbuf.at[i], dst, osem.at[i])
        for i, dst in enumerate((gate_o, up_o, down_o))
    ]
    for store in stores:
        store.start()

    def ag_copy(q, o, there, whose):
        h = lax.rem(there, 2)
        return pltpu.make_async_remote_copy(
            src_ref=trecv.at[h, pl.ds(q * ck, ck)], dst_ref=piece.at[q, whose],
            send_sem=ags.at[q, o], recv_sem=agr.at[q, o],
            device_id={"tp": there}, device_id_type=MESH,
        )

    def rs_copy(q, o, there, whose):
        return pltpu.make_async_remote_copy(
            src_ref=part.at[q, there], dst_ref=rsbuf.at[q, whose],
            send_sem=rss.at[q, o], recv_sem=rsr.at[q, o],
            device_id={"tp": there}, device_id_type=MESH,
        )

    def ahead(o):
        return lax.rem(tp + o, tps)

    def behind(o):
        return lax.rem(tp + tps - o, tps)

    def around(fn):
        loop(1, tps, fn)

    def gather(q):
        every(lambda h, k: t_copy(h, k, to(h, k)).wait_recv(), q * ck, (q + 1) * ck)
        around(lambda o: ag_copy(q, o, ahead(o), tp).start())
        piece[q, tp] = trecv[core, q * ck : (q + 1) * ck]

    def work(q):
        around(lambda o: ag_copy(q, o, ahead(o), behind(o)).wait_recv())
        rows = ck * slots
        acc = jnp.zeros((rows, gu.shape[1]), F32)
        for j in range(tps):
            acc += jnp.dot(
                piece[q, j].reshape(rows, width), gu[j * width : (j + 1) * width, :],
                preferred_element_type=F32,
            )
        f = gu.shape[1] // 4
        hidden = []
        for i in range(2):
            gate_v, up_v = acc[:, 2 * i * f : (2 * i + 1) * f], acc[:, (2 * i + 1) * f : (2 * i + 2) * f]
            hidden.append((gate_v / (1.0 + jnp.exp(-gate_v)) * up_v).astype(BF))
        hidden = jnp.concatenate(hidden, axis=1)
        for j in range(tps):
            term = lax.dot_general(
                hidden, dn[j * width : (j + 1) * width, :], (((1,), (1,)), ((), ())),
                preferred_element_type=F32,
            )
            part[q, j] = term.astype(BF).reshape(ck, slots, width)
        around(lambda o: rs_copy(q, o, ahead(o), tp).start())
        rsbuf[q, tp] = part[q, tp]

    def finish(q):
        around(lambda o: rs_copy(q, o, ahead(o), behind(o)).wait_recv())
        for h in range(2):
            total = rsbuf[q, h].astype(F32)
            for chip in range(1, tps // 2):
                total += rsbuf[q, 2 * chip + h].astype(F32)
            res[h, q * ck : (q + 1) * ck] = total.astype(BF)
        every(lambda h, k: r_copy(h, k, back(h, k), me).start(), q * ck, (q + 1) * ck)

    gather(0)
    exchange.wait_recv()
    f = wbuf.shape[-1]
    depth = gu.shape[0]
    for i, src in enumerate((wbuf, wother)):
        gu[:, 2 * i * f : (2 * i + 1) * f] = src[0].reshape(depth, f)
        gu[:, (2 * i + 1) * f : (2 * i + 2) * f] = src[1].reshape(depth, f)
        dn[:, i * f : (i + 1) * f] = src[2].reshape(depth, f)

    todo = []
    for q in range(nq):
        todo += [(2 * q + 0.0, gather, q), (2 * q + 1.1, work, q), (2 * q + 3.2, finish, q)]
    for _, step, q in sorted(todo, key=lambda item: item[0])[1:]:
        step(q)

    ret[me] = res[0, half - 1]
    every(lambda h, k: r_copy(h, k, back(h, k), to(h, k)).wait_recv())
    table = ret[...].reshape(n * slots, width)
    mix = jnp.zeros((tok_rows, width), F32)
    for i in range(2):
        rows = jnp.dot(onehot[i], table, preferred_element_type=F32)
        mix += rows * cols[:, 2 + i : 3 + i]
    mixed[...] = mix.astype(BF)

    for store in stores:
        store.wait()
    loop(1, n, lambda delta: w_to(delta).wait_send())
    every(lambda h, k: t_copy(h, k, to(h, k)).wait_send())
    every(lambda h, k: r_copy(h, k, back(h, k), me).wait_send())
    for o in range(1, groups):
        y_copy(o, lax.rem(grp + o, groups), grp).wait_send()
    exchange.wait_send()
    for q in range(nq):
        around(lambda o: ag_copy(q, o, ahead(o), tp).wait_send())
        around(lambda o: rs_copy(q, o, ahead(o), tp).wait_send())


def hand_on(*refs):
    count = (len(refs) - 2) // 3
    given, taken, held = (refs[i * count : (i + 1) * count] for i in range(3))
    isem, osem = refs[-2:]
    loads = [pltpu.make_async_copy(a, b, isem.at[i]) for i, (a, b) in enumerate(zip(given, held))]
    stores = [pltpu.make_async_copy(a, b, osem.at[i]) for i, (a, b) in enumerate(zip(held, taken))]
    for load in loads:
        load.start()
    for load, store in zip(loads, stores):
        load.wait()
        store.start()
    for store in stores:
        store.wait()


def body(chunks, tokens, norm_gain, gate_weight, up_weight, down_weight, ids, group_logits, pair_logits):
    experts, rows, f = gate_weight.shape
    tok_rows, width = tokens.shape
    n, groups, tps = lax.axis_size("fs"), lax.axis_size("grp"), lax.axis_size("tp")
    cap = 5 * tok_rows * 2 // (4 * experts)
    slots = -(-cap // 16) * 16
    half = n // 2
    ck = half // chunks
    share = rows // groups
    depth = n * rows

    def cut(weight):
        return weight.reshape(experts, groups, share, f)

    gain = norm_gain.reshape(1, rows)
    vmem = pl.BlockSpec(memory_space=pltpu.VMEM)
    hbm = pl.BlockSpec(memory_space=pl.ANY)
    whole = jax.ShapeDtypeStruct((n, groups, share, f), BF)
    dma = pltpu.SemaphoreType.DMA
    out = pl.pallas_call(
        functools.partial(kernel, (n, groups, tps, cap, slots, chunks, ck)),
        out_shape=(jax.ShapeDtypeStruct((tok_rows, width), BF), whole, whole, whole),
        in_specs=[hbm, vmem, hbm, hbm, hbm, vmem, vmem, vmem],
        out_specs=(vmem, hbm, hbm, hbm),
        name="experts",
        scratch_shapes=[
            pltpu.VMEM((groups, share, f), F32),
            pltpu.VMEM((3, n, share, f), F32),
            pltpu.VMEM((n, 3, share, f), BF),
            pltpu.VMEM((3, n, groups, share, f), BF),
            pltpu.VMEM((3, n, groups, share, f), BF),
            pltpu.VMEM((depth, 4 * f), BF),
            pltpu.VMEM((depth, 2 * f), BF),
            pltpu.VMEM((tok_rows, width), BF),
            pltpu.VMEM((n, slots, width), BF),
            pltpu.VMEM((2, half, slots, width), BF),
            pltpu.VMEM((chunks, tps, ck, slots, width), BF),
            pltpu.VMEM((chunks, tps, ck, slots, width), BF),
            pltpu.VMEM((chunks, tps, ck, slots, width), BF),
            pltpu.VMEM((2, half, slots, width), BF),
            pltpu.VMEM((n, slots, width), BF),
            pltpu.VMEM((2, tok_rows, n * slots), BF),
            pltpu.VMEM((tok_rows, 128), F32),
            pltpu.SemaphoreType.REGULAR((n,)), dma((4,)), dma((3,)),
            dma((n,)), dma((n,)),
            dma((2, half)), dma((2, half)),
            dma((2, half)), dma((2, half)),
            dma((groups,)), dma((groups,)),
            dma, dma,
            dma((chunks, tps)), dma((chunks, tps)),
            dma((chunks, tps)), dma((chunks, tps)),
        ],
        compiler_params=pltpu.CompilerParams(collective_id=0, has_side_effects=True),
    )(
        tokens, gain, cut(gate_weight), cut(up_weight), cut(down_weight),
        ids.T, group_logits.T, pair_logits.T,
    )
    shapes = [jax.ShapeDtypeStruct(a.shape, a.dtype) for a in out]
    mixed, gate_out, up_out, down_out = pl.pallas_call(
        hand_on,
        out_shape=shapes,
        in_specs=[hbm] * len(out),
        out_specs=[hbm] * len(out),
        scratch_shapes=[pltpu.VMEM(a.shape, a.dtype) for a in out] + [dma((len(out),)), dma((len(out),))],
    )(*out)
    return (mixed,) + tuple(w.reshape(1, depth, f) for w in (gate_out, up_out, down_out))


def solution(mesh, chunks=4):
    placed = (
        P(("grp", "fs"), "tp"),
        P("fs"),
        P(None, "fs", "tp"),
        P(None, "fs", "tp"),
        P(None, "fs", "tp"),
        P(("grp", "fs"), None),
        P(("grp", "fs"), None),
        P(("grp", "fs"), None),
    )
    return jax.shard_map(
        functools.partial(body, chunks),
        mesh=mesh,
        in_specs=placed,
        out_specs=(
            P(("grp", "fs"), "tp"),
            P(("grp", "fs"), None, "tp"),
            P(("grp", "fs"), None, "tp"),
            P(("grp", "fs"), None, "tp"),
        ),
        check_vma=False,
    )
```

```python
import functools

import jax
import jax.numpy as jnp
from jax import lax
from jax.experimental import pallas as pl
from jax.experimental.pallas import tpu as pltpu
from jax.sharding import PartitionSpec as P

MESH = pl.DeviceIdType.MESH
BF = jnp.bfloat16
F32 = jnp.float32


def kernel(
    cfg, tok_hbm, gain, gate_hbm, up_hbm, down_hbm, ids, glog, plog,
    mixed, gate_o, up_o, down_o,
    gains, wf, wstage, wbuf, wother, gu, dall, dn, tokv, outs, trecv, piece, hbuf, res, ret, onehot, cols,
    ready, lsem, osem, ws, wr, ts, tr, rs, rr, ys, yr, ds, dr, ns, nr, ags, agr, hs, hr, es, er,
):
    n, groups, tps, cap, slots, ck, order, plan = cfg
    half = n // 2
    tok_rows, width = tokv.shape
    me, grp, tp = lax.axis_index("fs"), lax.axis_index("grp"), lax.axis_index("tp")
    core = lax.rem(tp, 2)
    partner = tp + 1 - 2 * core

    loads = [
        pltpu.make_async_copy(src.at[:, grp], wf.at[i], lsem.at[i])
        for i, src in enumerate((gate_hbm, up_hbm, down_hbm))
    ]
    for load in loads:
        load.start()
    tok_load = pltpu.make_async_copy(tok_hbm, tokv, lsem.at[3])
    tok_load.start()

    barrier = pltpu.get_barrier_semaphore()
    rank = lax.rem(me + n - 1, n)

    def loop(lo, hi, fn):
        def one(i, c):
            fn(i)
            return c

        lax.fori_loop(lo, hi, one, 0)

    def greet(axis, there):
        pl.semaphore_signal(barrier, inc=1, device_id={axis: there}, device_id_type=MESH)

    loop(1, n - rank, lambda i: greet("fs", lax.rem(me + i, n)))
    loop(1, tps, lambda i: greet("tp", lax.rem(tp + i, tps)))
    loop(1, groups, lambda i: greet("grp", lax.rem(grp + i, groups)))

    rows = gain.shape[1]
    diagonal = lax.broadcasted_iota(jnp.int32, (rows, rows), 0) == lax.broadcasted_iota(jnp.int32, (rows, rows), 1)
    column = jnp.sum(jnp.where(diagonal, gain[...], 0.0), axis=1, keepdims=True)
    gains[...] = jnp.broadcast_to(column, (rows, gains.shape[2])).reshape(gains.shape)
    for i, load in enumerate(loads):
        load.wait()
        if i < 2:
            wstage[:, i] = (wf[i] * gains[grp][None]).astype(BF)
        else:
            wstage[:, i] = wf[i].astype(BF)
        wbuf[i, me, grp] = wstage[me, i]

    pl.semaphore_wait(barrier, rank + tps - 1 + groups - 1)

    def report(i):
        there = lax.rem(me + n - i, n)
        pl.semaphore_signal(ready.at[i], inc=1, device_id={"fs": there}, device_id_type=MESH)

    loop(1, rank + 1, report)

    def delta_of(h, k):
        return half - 1 - k if h == 0 else half + k

    def to(h, k):
        return lax.rem(me + delta_of(h, k), n)

    def back(h, k):
        return lax.rem(me + n - delta_of(h, k), n)

    def every(fn, lo=0, hi=half):
        def one(k, c):
            fn(0, k)
            fn(1, k)
            return c

        last = min(hi, half - 1)
        lax.fori_loop(lo, last, one, 0)
        if hi == half:
            fn(1, half - 1)

    def w_copy(delta, dst, src):
        return pltpu.make_async_remote_copy(
            src_ref=wstage.at[dst], dst_ref=wbuf.at[:, src, grp],
            send_sem=ws.at[delta], recv_sem=wr.at[delta],
            device_id={"fs": dst}, device_id_type=MESH,
        )

    def w_to(delta):
        return w_copy(delta, lax.rem(me + delta, n), me)

    def w_from(delta):
        return w_copy(delta, lax.rem(me + delta, n), lax.rem(me + n - delta, n))

    def t_copy(h, k, dst):
        return pltpu.make_async_remote_copy(
            src_ref=outs.at[dst], dst_ref=trecv.at[h, k],
            send_sem=ts.at[h, k], recv_sem=tr.at[h, k],
            device_id={"fs": dst}, device_id_type=MESH,
        )

    def r_copy(h, k, dst):
        return pltpu.make_async_remote_copy(
            src_ref=res.at[h, k], dst_ref=ret.at[h, k],
            send_sem=rs.at[h, k], recv_sem=rr.at[h, k],
            device_id={"fs": dst}, device_id_type=MESH,
        )

    loop(1, rank + 1, lambda i: w_to(n - i).start())

    exp_group = n // glog.shape[0]
    first, second = ids[0:1, :], ids[1:2, :]
    e_iota = lax.broadcasted_iota(jnp.int32, (n, tok_rows), 0)
    is0, is1 = e_iota == first, e_iota == second
    count = (is0 | is1).astype(F32).astype(BF)
    earlier = (
        lax.broadcasted_iota(jnp.int32, (tok_rows, tok_rows), 0)
        < lax.broadcasted_iota(jnp.int32, (tok_rows, tok_rows), 1)
    ).astype(F32).astype(BF)
    before = jnp.dot(count, earlier, preferred_element_type=F32)
    rank0 = jnp.sum(jnp.where(is0, before, 0.0), axis=0, keepdims=True)
    rank1 = jnp.sum(jnp.where(is1, before, 0.0), axis=0, keepdims=True)
    keep0, keep1 = rank0 < cap, rank1 < cap
    slot0 = jnp.where(keep0, first.astype(F32) * slots + rank0, -1.0)
    slot1 = jnp.where(keep1, second.astype(F32) * slots + rank1, -1.0)

    def place(expert, rank_in, keep):
        rel = jnp.where(expert >= me, expert - me, expert - me + n)
        spot = jnp.where(rel < half, half - 1 - rel, rel)
        return jnp.where(keep, spot.astype(F32) * slots + rank_in, -1.0)

    place0, place1 = place(first, rank0, keep0), place(second, rank1, keep1)

    group_exp = [jnp.exp(glog[g : g + 1, :]) for g in range(glog.shape[0])]
    chosen, total = jnp.zeros_like(slot0), jnp.zeros_like(slot0)
    for g, value in enumerate(group_exp):
        mine = (first >= g * exp_group) & (first < (g + 1) * exp_group)
        chosen += jnp.where(mine, value, 0.0)
        total += value
    chosen = chosen / total
    pair0, pair1 = jnp.exp(plog[0:1, :]), jnp.exp(plog[1:2, :])
    weight0 = jnp.where(keep0, pair0 / (pair0 + pair1) * chosen, 0.0)
    weight1 = jnp.where(keep1, pair1 / (pair0 + pair1) * chosen, 0.0)

    tok_load.wait()
    tokens = tokv[...]
    slot0i, slot1i = slot0.astype(jnp.int32), slot1.astype(jnp.int32)
    build = 4 * slots
    s_iota = lax.broadcasted_iota(jnp.int32, (build, tok_rows), 0)

    def fill(b, c):
        at = s_iota + b * build
        pick = ((at == slot0i) | (at == slot1i)).astype(F32).astype(BF)
        rows = jnp.dot(pick, tokens, preferred_element_type=F32).astype(BF)
        outs[pl.ds(b * 4, 4)] = rows.reshape(4, slots, width)
        return c

    lax.fori_loop(0, n // 4, fill, 0)

    def late(i):
        pl.semaphore_wait(ready.at[i], 1)
        w_to(i).start()

    loop(1, n - rank, late)
    for q in order:
        every(lambda h, k: t_copy(h, k, to(h, k)).start(), q * ck, (q + 1) * ck)
    trecv[0, half - 1] = outs[me]

    lines = lax.broadcasted_iota(jnp.int32, (128, tok_rows), 0)
    packed = jnp.zeros((128, tok_rows), F32)
    for i, row in enumerate((place0, place1, weight0, weight1)):
        packed = jnp.where(lines == i, row, packed)
    cols[...] = packed.T
    l_iota = lax.broadcasted_iota(jnp.int32, (tok_rows, n * slots), 1)
    for i in range(2):
        onehot[i] = (l_iota == cols[:, i : i + 1].astype(jnp.int32)).astype(F32).astype(BF)

    def delta_at(p):
        return jnp.where(lax.rem(p, 2) == 1, (p + 1) // 2, lax.rem(n - p // 2, n))

    def source_at(p):
        return lax.rem(me + n - delta_at(p), n)

    batch = n // yr.shape[1]

    def y_copy(o, p):
        spot = wbuf.at[:, source_at(p), grp]
        return pltpu.make_async_remote_copy(
            src_ref=spot, dst_ref=spot, send_sem=ys.at[o], recv_sem=yr.at[o, p // batch],
            device_id={"grp": lax.rem(grp + o, groups)}, device_id_type=MESH,
        )

    def d_copy(p, whose):
        at = source_at(p)
        return pltpu.make_async_remote_copy(
            src_ref=wbuf.at[0:2, at, whose], dst_ref=wother.at[:, at, whose], send_sem=ds, recv_sem=dr,
            device_id={"tp": partner}, device_id_type=MESH,
        )

    def pass_on(p):
        loop(1, groups, lambda o: y_copy(o, p).start())
        d_copy(p, grp).start()

    def landed(p):
        w_from(delta_at(p)).wait_recv()
        pass_on(p)

    pass_on(0)
    loop(1, n, landed)

    def shared(o):
        whose = lax.rem(grp + groups - o, groups)

        def some(b):
            blocks = wbuf.at[:, pl.ds(0, batch), 0]
            pltpu.make_async_copy(blocks, blocks, yr.at[o, b]).wait()
            loop(b * batch, (b + 1) * batch, lambda p: d_copy(p, whose).start())

        loop(0, n // batch, some)

    loop(1, groups, shared)
    stores = [
        pltpu.make_async_copy(wbuf.at[i], dst, osem.at[i])
        for i, dst in enumerate((gate_o, up_o, down_o))
    ]
    for store in stores:
        store.start()

    def ag_copy(q, o, there, whose):
        h = lax.rem(there, 2)
        return pltpu.make_async_remote_copy(
            src_ref=trecv.at[h, pl.ds(q * ck, ck)], dst_ref=piece.at[q, whose],
            send_sem=ags.at[q, o], recv_sem=agr.at[q, o],
            device_id={"tp": there}, device_id_type=MESH,
        )

    dn_src = dall.shape[1]

    def n_copy(o, there, whose):
        return pltpu.make_async_remote_copy(
            src_ref=wbuf.at[2, pl.ds(there * dn_src, dn_src)], dst_ref=dall.at[whose],
            send_sem=ns.at[o], recv_sem=nr.at[o],
            device_id={"tp": there}, device_id_type=MESH,
        )

    f = wbuf.shape[-1]
    chip = tp // 2
    chips = tps // 2

    def h_copy(q, o):
        spot = hbuf.at[q, chip, core]
        return pltpu.make_async_remote_copy(
            src_ref=spot, dst_ref=spot, send_sem=hs.at[q, o], recv_sem=hr.at[q, o],
            device_id={"tp": lax.rem(tp + 2 * o, tps)}, device_id_type=MESH,
        )

    def h_from(q, o):
        spot = hbuf.at[q, lax.rem(chip + chips - o, chips), core]
        return pltpu.make_async_remote_copy(
            src_ref=spot, dst_ref=spot, send_sem=hs.at[q, o], recv_sem=hr.at[q, o],
            device_id={"tp": lax.rem(tp + 2 * o, tps)}, device_id_type=MESH,
        )

    def e_copy(q, o, side):
        spot = hbuf.at[q, lax.rem(chip + chips - o, chips), side]
        return pltpu.make_async_remote_copy(
            src_ref=spot, dst_ref=spot, send_sem=es.at[q, o], recv_sem=er.at[q, o],
            device_id={"tp": partner}, device_id_type=MESH,
        )

    def ahead(o):
        return lax.rem(tp + o, tps)

    def behind(o):
        return lax.rem(tp + tps - o, tps)

    def around(fn):
        loop(1, tps, fn)

    def gather(q):
        every(lambda h, k: t_copy(h, k, to(h, k)).wait_recv(), q * ck, (q + 1) * ck)
        around(lambda o: ag_copy(q, o, ahead(o), tp).start())

    def block(j):
        return pl.ds(pl.multiple_of(j * width, width), width)

    def work(q):
        rows = ck * slots
        acc = jnp.dot(
            trecv[core, q * ck : (q + 1) * ck].reshape(rows, width), gu[block(tp), :],
            preferred_element_type=F32,
        )
        for o in range(1, tps):
            j = behind(o)
            ag_copy(q, o, ahead(o), j).wait_recv()
            acc += jnp.dot(
                piece[q, j].reshape(rows, width), gu[block(j), :], preferred_element_type=F32
            )
        f = gu.shape[1] // 4
        hidden = []
        for i in range(2):
            gate_v, up_v = acc[:, 2 * i * f : (2 * i + 1) * f], acc[:, (2 * i + 1) * f : (2 * i + 2) * f]
            hidden.append(gate_v / (1.0 + jnp.exp(-gate_v)) * up_v)
        low = jnp.where(core == 0, hidden[0], hidden[1])
        high = jnp.where(core == 0, hidden[1], hidden[0])
        hbuf[q, chip, core, :, 0:f] = low.astype(BF)
        hbuf[q, chip, core, :, f : 2 * f] = high.astype(BF)
        for o in range(1, chips):
            h_copy(q, o).start()
        e_copy(q, 0, core).start()

    def relay(q):
        for o in range(1, chips):
            h_from(q, o).wait_recv()
            e_copy(q, o, core).start()

    def join_down():
        around(lambda o: n_copy(o, ahead(o), behind(o)).wait_recv())
        for x in range(chips):
            for i in range(2):
                dn[x, :, i * f : (i + 1) * f] = dall[2 * x + i].reshape(width, f)

    def finish(q):
        for o in range(chips):
            e_copy(q, o, 1 - core).wait_recv()
        for h in range(2):
            total = jnp.zeros((ck * slots, width), F32)
            for x in range(chips):
                total += lax.dot_general(
                    hbuf[q, x, h], dn[x], (((1,), (1,)), ((), ())), preferred_element_type=F32
                )
            res[h, q * ck : (q + 1) * ck] = total.astype(BF).reshape(ck, slots, width)
        every(lambda h, k: r_copy(h, k, back(h, k)).start(), q * ck, (q + 1) * ck)

    around(lambda o: n_copy(o, ahead(o), tp).start())
    dall[tp] = wbuf[2, pl.ds(tp * dn_src, dn_src)]
    gather(order[0])
    pltpu.make_async_copy(wother, wother, dr).wait()
    depth = gu.shape[0]
    for i, src in enumerate((wbuf, wother)):
        gu[:, 2 * i * f : (2 * i + 1) * f] = src[0].reshape(depth, f)
        gu[:, (2 * i + 1) * f : (2 * i + 2) * f] = src[1].reshape(depth, f)

    steps = [gather, work, relay, finish]
    for at, step in plan:
        if (at, step) == (0, FINISH):
            join_down()
        steps[step](order[at])

    ret[0, half - 1] = res[0, half - 1]
    mix = jnp.zeros((tok_rows, width), F32)
    for q in order:
        every(lambda h, k: r_copy(h, k, back(h, k)).wait_recv(), q * ck, (q + 1) * ck)
        for h in range(2):
            table = ret[h, q * ck : (q + 1) * ck].reshape(ck * slots, width)
            start = (h * half + q * ck) * slots
            for i in range(2):
                rows = jnp.dot(
                    onehot[i, :, start : start + ck * slots], table, preferred_element_type=F32
                )
                mix += rows * cols[:, 2 + i : 3 + i]
    mixed[...] = mix.astype(BF)

    for store in stores:
        store.wait()
    loop(1, n, lambda delta: w_to(delta).wait_send())
    every(lambda h, k: t_copy(h, k, to(h, k)).wait_send())
    every(lambda h, k: r_copy(h, k, back(h, k)).wait_send())
    mine = wbuf.at[:, :, grp]
    loop(1, groups, lambda o: pltpu.make_async_copy(mine, mine, ys.at[o]).wait())
    pltpu.make_async_copy(wother, wother, ds).wait()
    around(lambda o: n_copy(o, ahead(o), tp).wait_send())
    for q in order:
        around(lambda o: ag_copy(q, o, ahead(o), tp).wait_send())
        for o in range(chips):
            if o:
                h_copy(q, o).wait_send()
            e_copy(q, o, core).wait_send()


GATHER, WORK, RELAY, FINISH = range(4)


def plan_of(chunks):
    plan = []
    for q in range(chunks):
        plan += [(q, GATHER), (q - 1, RELAY), (q - 1, FINISH), (q, WORK)] if q else [(0, WORK)]
    plan += [(chunks - 1, RELAY), (chunks - 1, FINISH)]
    return tuple(plan)


def hand_on(*refs):
    count = (len(refs) - 2) // 3
    given, taken, held = (refs[i * count : (i + 1) * count] for i in range(3))
    isem, osem = refs[-2:]
    loads = [pltpu.make_async_copy(a, b, isem.at[i]) for i, (a, b) in enumerate(zip(given, held))]
    stores = [pltpu.make_async_copy(a, b, osem.at[i]) for i, (a, b) in enumerate(zip(held, taken))]
    for load in loads:
        load.start()
    for load, store in zip(loads, stores):
        load.wait()
        store.start()
    for store in stores:
        store.wait()


def body(order, tokens, norm_gain, gate_weight, up_weight, down_weight, ids, group_logits, pair_logits):
    experts, rows, f = gate_weight.shape
    tok_rows, width = tokens.shape
    n, groups, tps = lax.axis_size("fs"), lax.axis_size("grp"), lax.axis_size("tp")
    cap = 5 * tok_rows * 2 // (4 * experts)
    slots = -(-cap // 16) * 16
    half = n // 2
    chunks = len(order)
    ck = half // chunks
    share = rows // groups
    depth = n * rows

    def cut(weight):
        return weight.reshape(experts, groups, share, f)

    gain = norm_gain.reshape(1, rows)
    vmem = pl.BlockSpec(memory_space=pltpu.VMEM)
    hbm = pl.BlockSpec(memory_space=pl.ANY)
    whole = jax.ShapeDtypeStruct((n, groups, share, f), BF)
    dma = pltpu.SemaphoreType.DMA
    out = pl.pallas_call(
        functools.partial(kernel, (n, groups, tps, cap, slots, ck, order, plan_of(chunks))),
        out_shape=(jax.ShapeDtypeStruct((tok_rows, width), BF), whole, whole, whole),
        in_specs=[hbm, vmem, hbm, hbm, hbm, vmem, vmem, vmem],
        out_specs=(vmem, hbm, hbm, hbm),
        name="experts",
        scratch_shapes=[
            pltpu.VMEM((groups, share, f), F32),
            pltpu.VMEM((3, n, share, f), F32),
            pltpu.VMEM((n, 3, share, f), BF),
            pltpu.VMEM((3, n, groups, share, f), BF),
            pltpu.VMEM((2, n, groups, share, f), BF),
            pltpu.VMEM((depth, 4 * f), BF),
            pltpu.VMEM((tps, n // tps, groups, share, f), BF),
            pltpu.VMEM((tps // 2, width, 2 * f), BF),
            pltpu.VMEM((tok_rows, width), BF),
            pltpu.VMEM((n, slots, width), BF),
            pltpu.VMEM((2, half, slots, width), BF),
            pltpu.VMEM((chunks, tps, ck, slots, width), BF),
            pltpu.VMEM((chunks, tps // 2, 2, ck * slots, 2 * f), BF),
            pltpu.VMEM((2, half, slots, width), BF),
            pltpu.VMEM((2, half, slots, width), BF),
            pltpu.VMEM((2, tok_rows, n * slots), BF),
            pltpu.VMEM((tok_rows, 128), F32),
            pltpu.SemaphoreType.REGULAR((n,)), dma((4,)), dma((3,)),
            dma((n,)), dma((n,)),
            dma((2, half)), dma((2, half)),
            dma((2, half)), dma((2, half)),
            dma((groups,)), dma((groups, 4)),
            dma, dma,
            dma((tps,)), dma((tps,)),
            dma((chunks, tps)), dma((chunks, tps)),
            dma((chunks, tps // 2)), dma((chunks, tps // 2)),
            dma((chunks, tps // 2)), dma((chunks, tps // 2)),
        ],
        compiler_params=pltpu.CompilerParams(collective_id=0, has_side_effects=True),
    )(
        tokens, gain, cut(gate_weight), cut(up_weight), cut(down_weight),
        ids.T, group_logits.T, pair_logits.T,
    )
    shapes = [jax.ShapeDtypeStruct(a.shape, a.dtype) for a in out]
    mixed, gate_out, up_out, down_out = pl.pallas_call(
        hand_on,
        out_shape=shapes,
        in_specs=[hbm] * len(out),
        out_specs=[hbm] * len(out),
        scratch_shapes=[pltpu.VMEM(a.shape, a.dtype) for a in out] + [dma((len(out),)), dma((len(out),))],
    )(*out)
    return (mixed,) + tuple(w.reshape(1, depth, f) for w in (gate_out, up_out, down_out))


def solution(mesh, order=(0, 1, 2, 3)):
    placed = (
        P(("grp", "fs"), "tp"),
        P("fs"),
        P(None, "fs", "tp"),
        P(None, "fs", "tp"),
        P(None, "fs", "tp"),
        P(("grp", "fs"), None),
        P(("grp", "fs"), None),
        P(("grp", "fs"), None),
    )
    return jax.shard_map(
        functools.partial(body, order),
        mesh=mesh,
        in_specs=placed,
        out_specs=(
            P(("grp", "fs"), "tp"),
            P(("grp", "fs"), None, "tp"),
            P(("grp", "fs"), None, "tp"),
            P(("grp", "fs"), None, "tp"),
        ),
        check_vma=False,
    )
```

```python
import functools

import jax
import jax.numpy as jnp
from jax import lax
from jax.experimental import pallas as pl
from jax.experimental.pallas import tpu as pltpu
from jax.sharding import PartitionSpec as P

MESH = pl.DeviceIdType.MESH
BF = jnp.bfloat16
F32 = jnp.float32


def kernel(
    cfg, tok_hbm, gain, gate_hbm, up_hbm, down_hbm, ids, glog, plog,
    mixed, gate_o, up_o, down_o,
    gains, wf, wstage, wbuf, wother, gu, dall, dn, tokv, outs, trecv, piece, hbuf, res, ret, onehot, cols,
    ready, lsem, osem, ws, wr, ts, tr, rs, rr, ys, yr, ds, dr, ns, nr, ags, agr, hs, hr, es, er,
):
    n, groups, tps, cap, slots, ck, order, plan = cfg
    half = n // 2
    tok_rows, width = tokv.shape
    me, grp, tp = lax.axis_index("fs"), lax.axis_index("grp"), lax.axis_index("tp")
    core = lax.rem(tp, 2)
    partner = tp + 1 - 2 * core

    loads = [
        pltpu.make_async_copy(src.at[:, grp], wf.at[i], lsem.at[i])
        for i, src in enumerate((gate_hbm, up_hbm, down_hbm))
    ]
    for load in loads:
        load.start()
    tok_load = pltpu.make_async_copy(tok_hbm, tokv, lsem.at[3])
    tok_load.start()

    barrier = pltpu.get_barrier_semaphore()
    rank = lax.rem(me + n - 1, n)

    def loop(lo, hi, fn):
        def one(i, c):
            fn(i)
            return c

        lax.fori_loop(lo, hi, one, 0)

    def greet(axis, there):
        pl.semaphore_signal(barrier, inc=1, device_id={axis: there}, device_id_type=MESH)

    loop(1, n - rank, lambda i: greet("fs", lax.rem(me + i, n)))
    loop(1, tps, lambda i: greet("tp", lax.rem(tp + i, tps)))
    loop(1, groups, lambda i: greet("grp", lax.rem(grp + i, groups)))

    rows = gain.shape[1]
    diagonal = lax.broadcasted_iota(jnp.int32, (rows, rows), 0) == lax.broadcasted_iota(jnp.int32, (rows, rows), 1)
    column = jnp.sum(jnp.where(diagonal, gain[...], 0.0), axis=1, keepdims=True)
    gains[...] = jnp.broadcast_to(column, (rows, gains.shape[2])).reshape(gains.shape)
    for i, load in enumerate(loads):
        load.wait()
        if i < 2:
            wstage[:, i] = (wf[i] * gains[grp][None]).astype(BF)
        else:
            wstage[:, i] = wf[i].astype(BF)
        wbuf[i, me, grp] = wstage[me, i]

    pl.semaphore_wait(barrier, rank + tps - 1 + groups - 1)

    def report(i):
        there = lax.rem(me + n - i, n)
        pl.semaphore_signal(ready.at[i], inc=1, device_id={"fs": there}, device_id_type=MESH)

    loop(1, rank + 1, report)

    def delta_of(h, k):
        return half - 1 - k if h == 0 else half + k

    def to(h, k):
        return lax.rem(me + delta_of(h, k), n)

    def back(h, k):
        return lax.rem(me + n - delta_of(h, k), n)

    def every(fn, lo=0, hi=half):
        def one(k, c):
            fn(0, k)
            fn(1, k)
            return c

        last = min(hi, half - 1)
        lax.fori_loop(lo, last, one, 0)
        if hi == half:
            fn(1, half - 1)

    def w_copy(delta, dst, src):
        return pltpu.make_async_remote_copy(
            src_ref=wstage.at[dst], dst_ref=wbuf.at[:, src, grp],
            send_sem=ws.at[delta], recv_sem=wr.at[delta],
            device_id={"fs": dst}, device_id_type=MESH,
        )

    def w_to(delta):
        return w_copy(delta, lax.rem(me + delta, n), me)

    def w_from(delta):
        return w_copy(delta, lax.rem(me + delta, n), lax.rem(me + n - delta, n))

    def t_copy(h, k, dst):
        return pltpu.make_async_remote_copy(
            src_ref=outs.at[dst], dst_ref=trecv.at[h, k],
            send_sem=ts.at[h, k], recv_sem=tr.at[h, k],
            device_id={"fs": dst}, device_id_type=MESH,
        )

    def r_copy(h, k, dst):
        return pltpu.make_async_remote_copy(
            src_ref=res.at[h, k], dst_ref=ret.at[h, k],
            send_sem=rs.at[h, k], recv_sem=rr.at[h, k],
            device_id={"fs": dst}, device_id_type=MESH,
        )

    loop(1, rank + 1, lambda i: w_to(n - i).start())

    exp_group = n // glog.shape[0]
    first, second = ids[0:1, :], ids[1:2, :]
    e_iota = lax.broadcasted_iota(jnp.int32, (n, tok_rows), 0)
    is0, is1 = e_iota == first, e_iota == second
    count = (is0 | is1).astype(F32).astype(BF)
    earlier = (
        lax.broadcasted_iota(jnp.int32, (tok_rows, tok_rows), 0)
        < lax.broadcasted_iota(jnp.int32, (tok_rows, tok_rows), 1)
    ).astype(F32).astype(BF)
    before = jnp.dot(count, earlier, preferred_element_type=F32)
    rank0 = jnp.sum(jnp.where(is0, before, 0.0), axis=0, keepdims=True)
    rank1 = jnp.sum(jnp.where(is1, before, 0.0), axis=0, keepdims=True)
    keep0, keep1 = rank0 < cap, rank1 < cap
    slot0 = jnp.where(keep0, first.astype(F32) * slots + rank0, -1.0)
    slot1 = jnp.where(keep1, second.astype(F32) * slots + rank1, -1.0)

    def place(expert, rank_in, keep):
        rel = jnp.where(expert >= me, expert - me, expert - me + n)
        spot = jnp.where(rel < half, half - 1 - rel, rel)
        return jnp.where(keep, spot.astype(F32) * slots + rank_in, -1.0)

    place0, place1 = place(first, rank0, keep0), place(second, rank1, keep1)

    group_exp = [jnp.exp(glog[g : g + 1, :]) for g in range(glog.shape[0])]
    chosen, total = jnp.zeros_like(slot0), jnp.zeros_like(slot0)
    for g, value in enumerate(group_exp):
        mine = (first >= g * exp_group) & (first < (g + 1) * exp_group)
        chosen += jnp.where(mine, value, 0.0)
        total += value
    chosen = chosen / total
    pair0, pair1 = jnp.exp(plog[0:1, :]), jnp.exp(plog[1:2, :])
    weight0 = jnp.where(keep0, pair0 / (pair0 + pair1) * chosen, 0.0)
    weight1 = jnp.where(keep1, pair1 / (pair0 + pair1) * chosen, 0.0)

    tok_load.wait()
    tokens = tokv[...]
    slot0i, slot1i = slot0.astype(jnp.int32), slot1.astype(jnp.int32)
    build = 4 * slots
    s_iota = lax.broadcasted_iota(jnp.int32, (build, tok_rows), 0)

    def fill(b, c):
        at = s_iota + b * build
        pick = ((at == slot0i) | (at == slot1i)).astype(F32).astype(BF)
        rows = jnp.dot(pick, tokens, preferred_element_type=F32).astype(BF)
        outs[pl.ds(b * 4, 4)] = rows.reshape(4, slots, width)
        return c

    lax.fori_loop(0, n // 4, fill, 0)

    def late(i):
        pl.semaphore_wait(ready.at[i], 1)
        w_to(i).start()

    loop(1, n - rank, late)
    for q in order:
        every(lambda h, k: t_copy(h, k, to(h, k)).start(), q * ck, (q + 1) * ck)
    trecv[0, half - 1] = outs[me]

    lines = lax.broadcasted_iota(jnp.int32, (128, tok_rows), 0)
    packed = jnp.zeros((128, tok_rows), F32)
    for i, row in enumerate((place0, place1, weight0, weight1)):
        packed = jnp.where(lines == i, row, packed)
    cols[...] = packed.T
    l_iota = lax.broadcasted_iota(jnp.int32, (tok_rows, n * slots), 1)
    for i in range(2):
        onehot[i] = (l_iota == cols[:, i : i + 1].astype(jnp.int32)).astype(F32).astype(BF)

    def delta_at(p):
        return jnp.where(lax.rem(p, 2) == 1, (p + 1) // 2, lax.rem(n - p // 2, n))

    def source_at(p):
        return lax.rem(me + n - delta_at(p), n)

    batch = n // yr.shape[1]

    def y_copy(o, p):
        spot = wbuf.at[:, source_at(p), grp]
        return pltpu.make_async_remote_copy(
            src_ref=spot, dst_ref=spot, send_sem=ys.at[o], recv_sem=yr.at[o, p // batch],
            device_id={"grp": lax.rem(grp + o, groups)}, device_id_type=MESH,
        )

    def d_copy(p, whose):
        at = source_at(p)
        return pltpu.make_async_remote_copy(
            src_ref=wbuf.at[0:2, at, whose], dst_ref=wother.at[:, at, whose], send_sem=ds, recv_sem=dr,
            device_id={"tp": partner}, device_id_type=MESH,
        )

    def pass_on(p):
        loop(1, groups, lambda o: y_copy(o, p).start())
        d_copy(p, grp).start()

    def landed(p):
        w_from(delta_at(p)).wait_recv()
        pass_on(p)

    def ag_copy(q, o, there, whose):
        h = lax.rem(there, 2)
        return pltpu.make_async_remote_copy(
            src_ref=trecv.at[h, pl.ds(q * ck, ck)], dst_ref=piece.at[q, whose],
            send_sem=ags.at[q, o], recv_sem=agr.at[q, o],
            device_id={"tp": there}, device_id_type=MESH,
        )

    dn_src = dall.shape[1]

    def n_copy(o, there, whose):
        return pltpu.make_async_remote_copy(
            src_ref=wbuf.at[2, pl.ds(there * dn_src, dn_src)], dst_ref=dall.at[whose],
            send_sem=ns.at[o], recv_sem=nr.at[o],
            device_id={"tp": there}, device_id_type=MESH,
        )

    f = wbuf.shape[-1]
    chip = tp // 2
    chips = tps // 2

    def h_copy(q, o):
        spot = hbuf.at[q, chip, core]
        return pltpu.make_async_remote_copy(
            src_ref=spot, dst_ref=spot, send_sem=hs.at[q, o], recv_sem=hr.at[q, o],
            device_id={"tp": lax.rem(tp + 2 * o, tps)}, device_id_type=MESH,
        )

    def h_from(q, o):
        spot = hbuf.at[q, lax.rem(chip + chips - o, chips), core]
        return pltpu.make_async_remote_copy(
            src_ref=spot, dst_ref=spot, send_sem=hs.at[q, o], recv_sem=hr.at[q, o],
            device_id={"tp": lax.rem(tp + 2 * o, tps)}, device_id_type=MESH,
        )

    def e_copy(q, o, side):
        spot = hbuf.at[q, lax.rem(chip + chips - o, chips), side]
        return pltpu.make_async_remote_copy(
            src_ref=spot, dst_ref=spot, send_sem=es.at[q, o], recv_sem=er.at[q, o],
            device_id={"tp": partner}, device_id_type=MESH,
        )

    def ahead(o):
        return lax.rem(tp + o, tps)

    def behind(o):
        return lax.rem(tp + tps - o, tps)

    def around(fn):
        loop(1, tps, fn)

    def gather(q):
        every(lambda h, k: t_copy(h, k, to(h, k)).wait_recv(), q * ck, (q + 1) * ck)
        around(lambda o: ag_copy(q, o, ahead(o), tp).start())

    pass_on(0)
    loop(1, n, landed)

    def shared(o):
        whose = lax.rem(grp + groups - o, groups)

        def some(b):
            blocks = wbuf.at[:, pl.ds(0, batch), 0]
            pltpu.make_async_copy(blocks, blocks, yr.at[o, b]).wait()
            loop(b * batch, (b + 1) * batch, lambda p: d_copy(p, whose).start())

        loop(0, n // batch, some)

    loop(1, groups, shared)
    gather(order[0])
    stores = [
        pltpu.make_async_copy(wbuf.at[i], dst, osem.at[i])
        for i, dst in enumerate((gate_o, up_o, down_o))
    ]
    for store in stores:
        store.start()

    def block(j):
        return pl.ds(pl.multiple_of(j * width, width), width)

    def work(q):
        rows = ck * slots
        acc = jnp.dot(
            trecv[core, q * ck : (q + 1) * ck].reshape(rows, width), gu[block(tp), :],
            preferred_element_type=F32,
        )
        for o in range(1, tps):
            j = behind(o)
            ag_copy(q, o, ahead(o), j).wait_recv()
            acc += jnp.dot(
                piece[q, j].reshape(rows, width), gu[block(j), :], preferred_element_type=F32
            )
        f = gu.shape[1] // 4
        hidden = []
        for i in range(2):
            gate_v, up_v = acc[:, 2 * i * f : (2 * i + 1) * f], acc[:, (2 * i + 1) * f : (2 * i + 2) * f]
            hidden.append(gate_v / (1.0 + jnp.exp(-gate_v)) * up_v)
        low = jnp.where(core == 0, hidden[0], hidden[1])
        high = jnp.where(core == 0, hidden[1], hidden[0])
        hbuf[q, chip, core, :, 0:f] = low.astype(BF)
        hbuf[q, chip, core, :, f : 2 * f] = high.astype(BF)
        for o in range(1, chips):
            h_copy(q, o).start()
        e_copy(q, 0, core).start()

    def relay(q):
        for o in range(1, chips):
            h_from(q, o).wait_recv()
            e_copy(q, o, core).start()

    def join_down():
        around(lambda o: n_copy(o, ahead(o), behind(o)).wait_recv())
        for x in range(chips):
            for i in range(2):
                dn[x, :, i * f : (i + 1) * f] = dall[2 * x + i].reshape(width, f)

    def side(q, h):
        lo, hi = q * ck, (q + 1) * ck
        total = jnp.zeros((ck * slots, width), F32)
        for x in range(chips):
            total += lax.dot_general(
                hbuf[q, x, h], dn[x], (((1,), (1,)), ((), ())), preferred_element_type=F32
            )
        res[h, lo:hi] = total.astype(BF).reshape(ck, slots, width)

        def send(k):
            delta = jnp.where(h == 0, half - 1 - k, half + k)
            r_copy(h, k, lax.rem(me + n - delta, n)).start()

        loop(lo, hi - jnp.where(h == 0, 1, 0) if hi == half else hi, send)

    def finish(q):
        side(q, core)
        for o in range(chips):
            e_copy(q, o, 1 - core).wait_recv()
        side(q, 1 - core)

    around(lambda o: n_copy(o, ahead(o), tp).start())
    dall[tp] = wbuf[2, pl.ds(tp * dn_src, dn_src)]
    pltpu.make_async_copy(wother, wother, dr).wait()
    depth = gu.shape[0]
    for i, src in enumerate((wbuf, wother)):
        gu[:, 2 * i * f : (2 * i + 1) * f] = src[0].reshape(depth, f)
        gu[:, (2 * i + 1) * f : (2 * i + 2) * f] = src[1].reshape(depth, f)

    steps = [gather, work, relay, finish]
    for at, step in plan:
        if (at, step) == (0, FINISH):
            join_down()
        steps[step](order[at])

    ret[0, half - 1] = res[0, half - 1]
    for store in stores:
        store.wait()
    loop(1, n, lambda delta: w_to(delta).wait_send())
    every(lambda h, k: t_copy(h, k, to(h, k)).wait_send())
    mine = wbuf.at[:, :, grp]
    loop(1, groups, lambda o: pltpu.make_async_copy(mine, mine, ys.at[o]).wait())
    pltpu.make_async_copy(wother, wother, ds).wait()
    around(lambda o: n_copy(o, ahead(o), tp).wait_send())
    for q in order:
        around(lambda o: ag_copy(q, o, ahead(o), tp).wait_send())
        for o in range(chips):
            if o:
                h_copy(q, o).wait_send()
            e_copy(q, o, core).wait_send()
    mix = jnp.zeros((tok_rows, width), F32)
    for q in order:
        every(lambda h, k: r_copy(h, k, back(h, k)).wait(), q * ck, (q + 1) * ck)
        for h in range(2):
            table = ret[h, q * ck : (q + 1) * ck].reshape(ck * slots, width)
            start = (h * half + q * ck) * slots
            for i in range(2):
                rows = jnp.dot(
                    onehot[i, :, start : start + ck * slots], table, preferred_element_type=F32
                )
                mix += rows * cols[:, 2 + i : 3 + i]
    mixed[...] = mix.astype(BF)


GATHER, WORK, RELAY, FINISH = range(4)


def plan_of(chunks):
    plan = []
    for q in range(chunks):
        plan += [(q, GATHER), (q - 1, RELAY), (q - 1, FINISH), (q, WORK)] if q else [(0, WORK)]
    plan += [(chunks - 1, RELAY), (chunks - 1, FINISH)]
    return tuple(plan)


def hand_on(*refs):
    count = (len(refs) - 2) // 3
    given, taken, held = (refs[i * count : (i + 1) * count] for i in range(3))
    isem, osem = refs[-2:]
    loads = [pltpu.make_async_copy(a, b, isem.at[i]) for i, (a, b) in enumerate(zip(given, held))]
    stores = [pltpu.make_async_copy(a, b, osem.at[i]) for i, (a, b) in enumerate(zip(held, taken))]
    for load in loads:
        load.start()
    for load, store in zip(loads, stores):
        load.wait()
        store.start()
    for store in stores:
        store.wait()


def body(order, tokens, norm_gain, gate_weight, up_weight, down_weight, ids, group_logits, pair_logits):
    experts, rows, f = gate_weight.shape
    tok_rows, width = tokens.shape
    n, groups, tps = lax.axis_size("fs"), lax.axis_size("grp"), lax.axis_size("tp")
    cap = 5 * tok_rows * 2 // (4 * experts)
    slots = -(-cap // 16) * 16
    half = n // 2
    chunks = len(order)
    ck = half // chunks
    share = rows // groups
    depth = n * rows

    def cut(weight):
        return weight.reshape(experts, groups, share, f)

    gain = norm_gain.reshape(1, rows)
    vmem = pl.BlockSpec(memory_space=pltpu.VMEM)
    hbm = pl.BlockSpec(memory_space=pl.ANY)
    whole = jax.ShapeDtypeStruct((n, groups, share, f), BF)
    dma = pltpu.SemaphoreType.DMA
    out = pl.pallas_call(
        functools.partial(kernel, (n, groups, tps, cap, slots, ck, order, plan_of(chunks))),
        out_shape=(jax.ShapeDtypeStruct((tok_rows, width), BF), whole, whole, whole),
        in_specs=[hbm, vmem, hbm, hbm, hbm, vmem, vmem, vmem],
        out_specs=(vmem, hbm, hbm, hbm),
        name="experts",
        scratch_shapes=[
            pltpu.VMEM((groups, share, f), F32),
            pltpu.VMEM((3, n, share, f), F32),
            pltpu.VMEM((n, 3, share, f), BF),
            pltpu.VMEM((3, n, groups, share, f), BF),
            pltpu.VMEM((2, n, groups, share, f), BF),
            pltpu.VMEM((depth, 4 * f), BF),
            pltpu.VMEM((tps, n // tps, groups, share, f), BF),
            pltpu.VMEM((tps // 2, width, 2 * f), BF),
            pltpu.VMEM((tok_rows, width), BF),
            pltpu.VMEM((n, slots, width), BF),
            pltpu.VMEM((2, half, slots, width), BF),
            pltpu.VMEM((chunks, tps, ck, slots, width), BF),
            pltpu.VMEM((chunks, tps // 2, 2, ck * slots, 2 * f), BF),
            pltpu.VMEM((2, half, slots, width), BF),
            pltpu.VMEM((2, half, slots, width), BF),
            pltpu.VMEM((2, tok_rows, n * slots), BF),
            pltpu.VMEM((tok_rows, 128), F32),
            pltpu.SemaphoreType.REGULAR((n,)), dma((4,)), dma((3,)),
            dma((n,)), dma((n,)),
            dma((2, half)), dma((2, half)),
            dma((2, half)), dma((2, half)),
            dma((groups,)), dma((groups, 4)),
            dma, dma,
            dma((tps,)), dma((tps,)),
            dma((chunks, tps)), dma((chunks, tps)),
            dma((chunks, tps // 2)), dma((chunks, tps // 2)),
            dma((chunks, tps // 2)), dma((chunks, tps // 2)),
        ],
        compiler_params=pltpu.CompilerParams(collective_id=0, has_side_effects=True),
    )(
        tokens, gain, cut(gate_weight), cut(up_weight), cut(down_weight),
        ids.T, group_logits.T, pair_logits.T,
    )
    shapes = [jax.ShapeDtypeStruct(a.shape, a.dtype) for a in out]
    mixed, gate_out, up_out, down_out = pl.pallas_call(
        hand_on,
        out_shape=shapes,
        in_specs=[hbm] * len(out),
        out_specs=[hbm] * len(out),
        scratch_shapes=[pltpu.VMEM(a.shape, a.dtype) for a in out] + [dma((len(out),)), dma((len(out),))],
    )(*out)
    return (mixed,) + tuple(w.reshape(1, depth, f) for w in (gate_out, up_out, down_out))


def solution(mesh, order=(0, 1, 2, 3)):
    placed = (
        P(("grp", "fs"), "tp"),
        P("fs"),
        P(None, "fs", "tp"),
        P(None, "fs", "tp"),
        P(None, "fs", "tp"),
        P(("grp", "fs"), None),
        P(("grp", "fs"), None),
        P(("grp", "fs"), None),
    )
    return jax.shard_map(
        functools.partial(body, order),
        mesh=mesh,
        in_specs=placed,
        out_specs=(
            P(("grp", "fs"), "tp"),
            P(("grp", "fs"), None, "tp"),
            P(("grp", "fs"), None, "tp"),
            P(("grp", "fs"), None, "tp"),
        ),
        check_vma=False,
    )
```
